32 devices in a mesh: sp: 8 (over z, y), tp: 4 (over x, core).
Axes of the slice: x: 2, y: 2, z: 4, core: 2. Of those that a mesh axis runs over, the one named last changes fastest.
Arguments:
- middle_stream: bfloat16 [1536, 2048], P('sp', 'tp'), may hold values from -6 to 6
- output_gradient: bfloat16 [1536, 2048], P('sp', 'tp'), may hold values from -6 to 6
- routes: int32 [1536, 2], P('sp'), may hold values from 0 to 7, all different within a row; in each aligned block of 192 rows (0 to 191, 192 to 383, ...) at most 72 rows name the same one
- chosen_expert_weight: float32 [1536, 2], P('sp'), may hold values from 0.2 to 1
- expert_gate_weight: bfloat16 [8, 2048, 3584], P('sp', None, 'tp'), may hold values from -0.125 to 0.125
- expert_up_weight: bfloat16 [8, 2048, 3584], P('sp', None, 'tp'), may hold values from -0.125 to 0.125
- expert_down_weight: bfloat16 [8, 3584, 2048], P('sp', 'tp'), may hold values from -0.09375 to 0.09375
- recurrent_output_weight: bfloat16 [2048, 1024], P(None, 'tp'), may hold values from -0.1875 to 0.1875
- recurrence_input: bfloat16 [1536, 1024], P('sp', 'tp'), may hold values from -8 to 8
- output_gate_logits: bfloat16 [1536, 1024], P('sp', 'tp'), may hold values from -6 to 6
- recurrence_gate_weight: bfloat16 [8, 128, 128], replicated, may hold values from -0.5 to 0.5
- input_gate_weight: bfloat16 [8, 128, 128], replicated, may hold values from -0.5 to 0.5
- channel_decay_param: float32 [1024], P('tp'), may hold values from 4 to 13
- extra_log_decay: float32 [1536, 1024], P('sp', 'tp'), may hold values from -0.7 to 0
Outputs:
- grad_gate: bfloat16 [8, 2048, 3584], P('sp', None, 'tp')
- grad_up: bfloat16 [8, 2048, 3584], P('sp', None, 'tp')
- grad_down: bfloat16 [8, 3584, 2048], P('sp', 'tp')
- grad_out_proj: float32 [2048, 1024], P('sp', 'tp')
- grad_input: float32 [1536, 1024], P('sp', 'tp')
- grad_gate_pre: float32 [1536, 1024], P('sp', 'tp')
The draws below stay inside these ranges and needn't reach their ends.
Inputs may be any that keep to these rules, and one draw needn't show every extreme that they name: `routes`: in the rows of one index of sp no expert is named more than 72 times, a bound that some block reaches in some of them; the entries of a row differ.
All inputs are finite; a program needn't handle non-finite values.
Results may differ from the reference program's by a relative error of at most 0.017.
Values may be sent and summed in bfloat16 or wider, within the bound.
A program may use at most 128 MiB of HBM per device.

```python
import math
import jax
import jax.numpy as jnp
import numpy as np
from jax import lax

D = 2048
FF = 3584
BLOCKS = 8
BW = 128
TOP = 2
TOK_DEV = 192
CHANNEL_COUNT = 1024
SEQUENCE_TOKENS = 1536
EXPERTS = 8
CAP = 72
N_SP = 8
N_TP = 4


def draw_recurrence_input(key, part):
    initial_key, second_key = jax.random.split(jax.random.fold_in(key, 11))
    base_draw = jnp.clip(jax.random.normal(initial_key, (SEQUENCE_TOKENS, CHANNEL_COUNT), jnp.float32), -4.0, 4.0)
    factor = jnp.exp(jax.random.uniform(second_key, (SEQUENCE_TOKENS // TOK_DEV, 1, 1), jnp.float32, math.log(0.5), math.log(2.0)))
    scaled = (base_draw.reshape(SEQUENCE_TOKENS // TOK_DEV, TOK_DEV, CHANNEL_COUNT) * factor).reshape(SEQUENCE_TOKENS, CHANNEL_COUNT)
    return scaled.astype(jnp.bfloat16)


def draw_channel_decay_param(key, part):
    initial_key, second_key, third_key = jax.random.split(jax.random.fold_in(key, 23), 3)
    fast_share = 0.5
    fast_pick = jax.random.uniform(initial_key, (CHANNEL_COUNT,), jnp.float32) < fast_share
    fast_rate = jnp.exp(jax.random.uniform(second_key, (CHANNEL_COUNT,), jnp.float32, math.log(0.003), math.log(0.01)))
    slow_rate = jnp.exp(jax.random.uniform(third_key, (CHANNEL_COUNT,), jnp.float32, math.log(0.05), math.log(0.3))) / SEQUENCE_TOKENS
    chosen = jnp.where(fast_pick, fast_rate, slow_rate)
    return (-jnp.log(jnp.expm1(chosen))).astype(jnp.float32)


def draw_extra_log_decay(key, part):
    initial_key, second_key = jax.random.split(jax.random.fold_in(key, 37))
    spike_mask = jax.random.uniform(initial_key, (SEQUENCE_TOKENS, CHANNEL_COUNT), jnp.float32) < 4.0 / SEQUENCE_TOKENS
    loss_history = jax.random.uniform(second_key, (SEQUENCE_TOKENS, CHANNEL_COUNT), jnp.float32, math.log(0.5), math.log(0.8))
    return jnp.where(spike_mask, loss_history, 0.0).astype(jnp.float32)


def strengthened(array, key, source, target, shards_of, factor):
    owner, partner = [(jnp.arange(array.shape[axis_at]) // (array.shape[axis_at] // shards_of)).reshape([-1 if axis == axis_at else 1 for axis in range(array.ndim)]) for axis_at in (source, target)]
    chosen = jax.random.permutation(key, shards_of)[partner]
    strong = (owner == chosen) | (owner == (partner + shards_of // 2) % shards_of)
    return jnp.where(strong, factor * array, array)


def steps_of(key, shape, cuts, smallest, top_value):
    loudness = 1.0
    for axis_at, shards_of in cuts:
        draws = jax.random.uniform(jax.random.fold_in(jax.random.fold_in(key, 6), axis_at), (shards_of,), jnp.float32, smallest / len(cuts), top_value / len(cuts))
        loudness = loudness * jnp.repeat(jnp.exp(draws), shape[axis_at] // shards_of).reshape((-1,) + (1,) * (len(shape) - 1 - axis_at))
    return loudness


def shared_out(key, own, number, rows, number_of, top, reach, skew):
    ranking = jax.random.permutation(key, number_of)
    heavy_load, ordinary = portions_of(number_of, rows * top, reach, skew, True), portions_of(number_of, rows * top, reach, skew, False)
    places = jnp.arange(number_of)

    def named(tallies, turn):
        used = int((tallies > 0).sum())
        fixed = max(1, used // 4)
        shifted = fixed + (places - fixed + turn * (used - fixed)) % max(1, number_of - fixed)
        return jnp.zeros((number_of,), jnp.int32).at[ranking[jnp.where(places < fixed, places, shifted)]].set(jnp.asarray(tallies, jnp.int32))

    tallies = jnp.where(number % 4 == 0, named(heavy_load, number // 4), named(ordinary, number - number // 4 - 1))
    mixed = jax.random.permutation(jax.random.fold_in(own, 3), number_of)
    source_of, taker = mixed[0:number_of // 2 * 2:2], mixed[1:number_of // 2 * 2:2]
    slack = jnp.minimum(tallies[source_of] - 1, reach - tallies[taker]) // 2
    slack = jnp.where((source_of == ranking[0]) | (taker == ranking[0]) | (tallies[taker] == 0), 0, jnp.maximum(slack, 0))
    shifted = jax.random.randint(jax.random.fold_in(own, 4), (number_of // 2,), 0, 1 << 20) % (slack + 1)
    tallies = tallies.at[source_of].add(-shifted).at[taker].add(shifted)
    labels = jnp.searchsorted(jnp.cumsum(tallies), jnp.arange(rows * top), side="right").astype(jnp.int32)
    listing = labels.reshape(top, rows).T
    listing = listing[jax.random.permutation(jax.random.fold_in(own, 1), rows)]
    turn = jax.random.randint(jax.random.fold_in(own, 2), (rows, 1), 0, top)
    return jnp.take_along_axis(listing, (jnp.arange(top)[None, :] + turn) % top, axis=1)


def portions_of(amount, total, bound, slope, full):
    portions = [(1 << 20) // math.isqrt(grade ** slope) + 1 for grade in range(1, amount + 1)]
    largest = bound if full else min(bound, max(-(-total // amount), total * portions[0] // sum(portions)))
    least = 1 if total - largest >= amount - 1 else 0
    holding, spare = [largest] + [least] * (amount - 1), total - largest - least * (amount - 1)
    while spare > 0:
        candidates = [i for i in range(1, amount) if holding[i] < largest] or [i for i in range(1, amount) if holding[i] < bound]
        whole, budget = sum([portions[i] for i in candidates]), spare
        for i in candidates:
            more = min(bound - holding[i], max(1, budget * portions[i] // whole), spare)
            holding[i] = holding[i] + more
            spare = spare - more
    return np.array(holding)


def bell_draw(stream_key, dims, width, bound, cuts=(), kind=jnp.bfloat16):
    array = jax.random.normal(stream_key, dims, jnp.float32) * width
    if len(cuts) > 0:
        array = steps_of(stream_key, dims, cuts, -0.22, 0.18) * array
    return jnp.clip(array, min=-bound, max=bound).astype(kind)


def noise_with(rng, dims, width, most, cuts, heavy, kind=jnp.bfloat16):
    array = width * jax.random.normal(rng, dims, jnp.float32)
    if cuts:
        array = array * steps_of(rng, dims, cuts, -0.22, 0.18)
    return jnp.clip(strengthened(array, jax.random.fold_in(rng, 3), *heavy), -most, most).astype(kind)


def setup_inputs(seed: int = 0) -> dict:
    streams_of = jax.random.split(jax.random.key(seed), 15)
    middle_stream = bell_draw(streams_of[0], (SEQUENCE_TOKENS, D), 1.0, 6.0, ((0, 8), (1, 4)))
    output_gradient = noise_with(streams_of[1], (SEQUENCE_TOKENS, D), 1.0, 6.0, ((0, 8), (1, 4)), (0, 1, 8, 2.0))
    routes_keys = jax.random.split(jax.random.fold_in(streams_of[2], 1), SEQUENCE_TOKENS // TOK_DEV)
    routes_turns = jax.random.permutation(jax.random.fold_in(streams_of[2], 3), SEQUENCE_TOKENS // TOK_DEV)
    routes = jax.vmap(lambda own, number: shared_out(jax.random.fold_in(streams_of[2], 2), own, number, TOK_DEV, EXPERTS, TOP, CAP, 1))(routes_keys, routes_turns).reshape((SEQUENCE_TOKENS, TOP))
    chosen_expert_weight = jnp.clip(0.2 + 0.8 * jax.random.uniform(streams_of[3], (SEQUENCE_TOKENS, TOP), jnp.float32) ** steps_of(streams_of[3], (SEQUENCE_TOKENS, TOP), ((0, 8),), -0.2, 0.2), 0.2, 1.0)
    expert_gate_weight = bell_draw(streams_of[4], (EXPERTS, D, FF), D ** -0.5, 0.125, ((0, 8), (2, 4)))
    expert_up_weight = bell_draw(streams_of[5], (EXPERTS, D, FF), D ** -0.5, 0.125, ((0, 8), (2, 4)))
    expert_down_weight = bell_draw(streams_of[6], (EXPERTS, FF, D), FF ** -0.5, 0.09375, ((0, 8), (1, 4)))
    recurrent_output_weight = bell_draw(streams_of[7], (D, CHANNEL_COUNT), CHANNEL_COUNT ** -0.5, 0.1875, ((1, 4),))
    recurrence_input = draw_recurrence_input(jax.random.fold_in(streams_of[14], 71), 0)
    output_gate_logits = bell_draw(streams_of[9], (SEQUENCE_TOKENS, CHANNEL_COUNT), 1.0, 6.0, ((0, 8), (1, 4)))
    recurrence_gate_weight = bell_draw(streams_of[10], (BLOCKS, BW, BW), BW ** -0.5, 0.5)
    input_gate_weight = bell_draw(streams_of[11], (BLOCKS, BW, BW), BW ** -0.5, 0.5)
    channel_decay_param = draw_channel_decay_param(jax.random.fold_in(streams_of[14], 71), 0)
    extra_log_decay = draw_extra_log_decay(jax.random.fold_in(streams_of[14], 71), 0)
    return {"middle_stream": middle_stream, "output_gradient": output_gradient, "routes": routes, "chosen_expert_weight": chosen_expert_weight, "expert_gate_weight": expert_gate_weight, "expert_up_weight": expert_up_weight, "expert_down_weight": expert_down_weight, "recurrent_output_weight": recurrent_output_weight, "recurrence_input": recurrence_input, "output_gate_logits": output_gate_logits, "recurrence_gate_weight": recurrence_gate_weight, "input_gate_weight": input_gate_weight, "channel_decay_param": channel_decay_param, "extra_log_decay": extra_log_decay}


def combine_linear(earlier, latter):
    return (earlier[0] * latter[0], latter[0] * earlier[1] + latter[1])

def linear_scan(factor, driven):
    return lax.associative_scan(combine_linear, (factor, driven), axis=0)

def gelu_parts(output_gate_logits):
    gate_float = output_gate_logits.astype(jnp.float32)
    return jax.jvp(jax.nn.gelu, (gate_float,), (jnp.ones_like(gate_float),))

def expert_backward(inputs, cotangent, gate_weight, up_weight, down_weight):
    gate_act = jnp.dot(inputs, gate_weight, preferred_element_type=jnp.float32)
    up_act = jnp.dot(inputs, up_weight, preferred_element_type=jnp.float32)
    sigmoid_gate = jax.nn.sigmoid(gate_act)
    silu_act = gate_act * sigmoid_gate
    hidden = (silu_act * up_act).astype(jnp.bfloat16)
    d_hidden = lax.dot_general(cotangent, down_weight, (((1,), (1,)), ((), ())), preferred_element_type=jnp.float32)
    grad_down = lax.dot_general(hidden, cotangent, (((0,), (0,)), ((), ())), preferred_element_type=jnp.float32)
    d_gate = (d_hidden * up_act * sigmoid_gate * (1.0 + gate_act * (1.0 - sigmoid_gate))).astype(jnp.bfloat16)
    d_up = (d_hidden * silu_act).astype(jnp.bfloat16)
    grad_gate = lax.dot_general(inputs, d_gate, (((0,), (0,)), ((), ())), preferred_element_type=jnp.float32)
    grad_up = lax.dot_general(inputs, d_up, (((0,), (0,)), ((), ())), preferred_element_type=jnp.float32)
    return (grad_gate.astype(jnp.bfloat16), grad_up.astype(jnp.bfloat16), grad_down.astype(jnp.bfloat16), d_gate, d_up)

def reference(middle_stream, output_gradient, routes, chosen_expert_weight, expert_gate_weight, expert_up_weight, expert_down_weight, recurrent_output_weight, recurrence_input, output_gate_logits, recurrence_gate_weight, input_gate_weight, channel_decay_param, extra_log_decay):
    tokens, model_width = middle_stream.shape
    top_count = routes.shape[1]
    routed = routes.reshape(-1)
    onehot = (routed[:, None] == jnp.arange(EXPERTS, dtype=jnp.int32)[None, :]).astype(jnp.int32)
    onehot = onehot.reshape(N_SP, TOK_DEV * top_count, EXPERTS)
    slot_rank = (lax.optimization_barrier(jnp.sum(jnp.cumsum(onehot, axis=1) * onehot, axis=2)) - 1).reshape(-1)
    source = jnp.arange(tokens * top_count, dtype=jnp.int32) // (TOK_DEV * top_count)
    buffer_place = (source * CAP + slot_rank).astype(jnp.int32)
    slot_table = jnp.full((EXPERTS, N_SP * CAP), tokens * top_count, jnp.int32)
    slot_table = slot_table.at[routed, buffer_place].set(jnp.arange(tokens * top_count, dtype=jnp.int32))
    zero_row = jnp.zeros((1, model_width), jnp.bfloat16)
    pair_rows = jnp.broadcast_to(middle_stream[:, None, :], (tokens, top_count, model_width)).reshape(-1, model_width)
    pair_rows = jnp.concatenate([pair_rows, zero_row], axis=0)
    pair_cot = (chosen_expert_weight[:, :, None] * output_gradient.astype(jnp.float32)[:, None, :]).astype(jnp.bfloat16)
    pair_cot = jnp.concatenate([pair_cot.reshape(-1, model_width), zero_row], axis=0)

    def one_expert(packed):
        table_row, gate_weight, up_weight, down_weight = packed
        inputs = pair_rows[table_row]
        cotangent = pair_cot[table_row]
        grad_gate, grad_up, grad_down, d_gate, d_up = expert_backward(inputs, cotangent, gate_weight, up_weight, down_weight)
        slot_rows = inputs.shape[0]
        quarter = gate_weight.shape[1] // N_TP
        gate_q = d_gate.astype(jnp.float32).reshape(slot_rows, N_TP, quarter)
        up_q = d_up.astype(jnp.float32).reshape(slot_rows, N_TP, quarter)
        gate_wq = gate_weight.astype(jnp.float32).reshape(model_width, N_TP, quarter)
        up_wq = up_weight.astype(jnp.float32).reshape(model_width, N_TP, quarter)
        partial_value = jnp.einsum('rqf,dqf->qrd', gate_q, gate_wq) + jnp.einsum('rqf,dqf->qrd', up_q, up_wq)
        rounded = lax.optimization_barrier(partial_value.astype(jnp.bfloat16)).astype(jnp.float32)
        slot_grad = lax.optimization_barrier(jnp.sum(rounded, axis=0)).astype(jnp.bfloat16)
        return (grad_gate, grad_up, grad_down, slot_grad)
    grad_gate, grad_up, grad_down, slot_grad = lax.map(one_expert, (slot_table, expert_gate_weight, expert_up_weight, expert_down_weight))
    slot_back = jnp.zeros((tokens * top_count + 1, model_width), jnp.bfloat16)
    slot_back = slot_back.at[slot_table.reshape(-1)].set(slot_grad.reshape(-1, model_width))
    arrived = slot_back[:-1].astype(jnp.float32).reshape(tokens, top_count, model_width)
    residual_grad = (output_gradient.astype(jnp.float32) + lax.optimization_barrier(jnp.sum(arrived, axis=1))).astype(jnp.bfloat16)
    mixer_grad = jnp.dot(residual_grad, recurrent_output_weight, preferred_element_type=jnp.float32)
    channels = recurrence_input.shape[1]
    blocks, block_width = (recurrence_gate_weight.shape[0], recurrence_gate_weight.shape[1])
    u_float = recurrence_input.astype(jnp.float32)
    u_blocks = u_float.reshape(tokens, blocks, block_width)
    forget_gate = jax.nn.sigmoid(jnp.einsum('tnb,nbc->tnc', u_blocks, recurrence_gate_weight.astype(jnp.float32)).reshape(tokens, channels))
    admit_gate = jax.nn.sigmoid(jnp.einsum('tnb,nbc->tnc', u_blocks, input_gate_weight.astype(jnp.float32)).reshape(tokens, channels))
    baseline_rate = jax.nn.softplus(-channel_decay_param)
    decay_logarithm = -8.0 * forget_gate * baseline_rate[None, :] + extra_log_decay
    decay_step = jnp.exp(decay_logarithm)
    input_scale = jnp.sqrt(-jnp.expm1(2.0 * decay_logarithm))
    driven = u_float * admit_gate * input_scale
    _, states = linear_scan(decay_step, driven)
    prev_states = jnp.concatenate([jnp.zeros((1, channels), jnp.float32), states[:-1]], axis=0)
    gelu_val, gelu_der = gelu_parts(output_gate_logits)
    lru_out = (states * gelu_val).astype(jnp.bfloat16)
    grad_out_proj = lax.dot_general(residual_grad, lru_out, (((0,), (0,)), ((), ())), preferred_element_type=jnp.float32)
    grad_gate_pre = mixer_grad * states * gelu_der
    state_in = mixer_grad * gelu_val
    next_decay = jnp.concatenate([decay_step[1:], jnp.zeros((1, channels), jnp.float32)], axis=0)
    _, flipped = linear_scan(next_decay[::-1], state_in[::-1])
    state_grad = flipped[::-1]
    d_log = state_grad * (prev_states * decay_step - u_float * admit_gate * decay_step * decay_step / input_scale)
    d_recall = (d_log * (-8.0 * baseline_rate[None, :]) * forget_gate * (1.0 - forget_gate)).astype(jnp.bfloat16)
    d_admit = (state_grad * u_float * input_scale * admit_gate * (1.0 - admit_gate)).astype(jnp.bfloat16)
    back_recall = jnp.einsum('tnc,nbc->tnb', d_recall.astype(jnp.float32).reshape(tokens, blocks, block_width), recurrence_gate_weight.astype(jnp.float32))
    back_admit = jnp.einsum('tnc,nbc->tnb', d_admit.astype(jnp.float32).reshape(tokens, blocks, block_width), input_gate_weight.astype(jnp.float32))
    grad_input = state_grad * admit_gate * input_scale + (back_recall + back_admit).reshape(tokens, channels)
    return (grad_gate, grad_up, grad_down, grad_out_proj, grad_input, grad_gate_pre)
```

```python
import functools

import jax
import jax.numpy as jnp
from jax import lax
from jax.experimental import pallas as pl
from jax.experimental.pallas import tpu as pltpu
from jax.sharding import PartitionSpec as P

MESH = pl.DeviceIdType.MESH


def partner(t, stage, m):
    d = m >> (stage + 1)
    return t + d * (1 - 2 * ((t // d) % 2))


def held_columns(t, stage, m):
    if stage == 0:
        return [t]
    return held_columns(t, stage - 1, m) + held_columns(partner(t, stage - 1, m), stage - 1, m)


def greet(peers):
    barrier = pltpu.get_barrier_semaphore()
    for peer in peers:
        pl.semaphore_signal(barrier, inc=1, device_id=peer, device_id_type=MESH)
    pl.semaphore_wait(barrier, len(peers))


def remote(src, dst, send_sem, recv_sem, peer):
    return pltpu.make_async_remote_copy(
        src_ref=src,
        dst_ref=dst,
        send_sem=send_sem,
        recv_sem=recv_sem,
        device_id=peer,
        device_id_type=MESH,
    )


def shifted(value, k, fill, reverse):
    pad = jnp.full((k, value.shape[1]), fill, value.dtype)
    if reverse:
        return jnp.concatenate([value[k:], pad], axis=0)
    return jnp.concatenate([pad, value[:-k]], axis=0)


def local_scan(gain, term, reverse):
    k = 1
    while k < gain.shape[0]:
        term = term + gain * shifted(term, k, 0.0, reverse)
        gain = gain * shifted(gain, k, 1.0, reverse)
        k *= 2
    return gain, term


def dispatch_kernel(
    n,
    m,
    send_ref,
    decay_ref,
    driven_ref,
    out_ref,
    states_ref,
    prev_ref,
    gain_buf,
    car_send,
    car_buf,
    a2a_send,
    a2a_recv,
    tp_send,
    tp_recv,
    car_ssem,
    car_rsem,
    self_sem,
):
    s, t = lax.axis_index("sp"), lax.axis_index("tp")
    feat = send_ref.shape[3]
    stages = m.bit_length() - 1
    greet(
        [{"sp": lax.rem(s + k, n)} for k in range(1, n)]
        + [{"tp": partner(t, j, m)} for j in range(stages)]
    )

    def block(src, col):
        return out_ref.at[:, src, :, pl.ds(pl.multiple_of(col * feat, feat), feat)]

    first = []
    own = pltpu.make_async_copy(send_ref.at[:, s], block(s, t), self_sem)
    own.start()
    for k in range(1, n):
        dst = lax.rem(s + k, n)
        copy = remote(
            send_ref.at[:, dst], block(s, t), a2a_send.at[k], a2a_recv.at[k], {"sp": dst}
        )
        copy.start()
        first.append(copy)

    pushed = []

    def push(k, stage, i, col):
        src = lax.rem(s + n - k, n)
        at = 2**stage - 1 + i
        copy = remote(
            block(src, col),
            block(src, col),
            tp_send.at[at, k],
            tp_recv.at[at, k],
            {"tp": partner(t, stage, m)},
        )
        copy.start()
        pushed.append(copy)

    def arrived(k, stage):
        src = lax.rem(s + n - k, n)
        cols = held_columns(partner(t, stage, m), stage, m)
        for i, col in enumerate(cols):
            at = 2**stage - 1 + i
            remote(
                block(src, col),
                block(src, col),
                tp_send.at[at, k],
                tp_recv.at[at, k],
                {"tp": partner(t, stage, m)},
            ).wait_recv()
            for later in range(stage + 1, stages):
                push(k, later, 2**stage + i, col)

    def forward(k):
        if k == 0:
            own.wait()
        else:
            first[k - 1].wait_recv()
        for stage in range(stages):
            push(k, stage, 0, t)

    forward(0)
    gain, term = local_scan(decay_ref[...], driven_ref[...], False)
    gain_buf[...] = gain
    states_ref[...] = term
    rows = gain.shape[0]
    car_send[0:1] = gain[rows - 1 : rows]
    car_send[1:2] = term[rows - 1 : rows]
    forward(1)
    carries = []
    for k in range(1, n):
        copy = remote(
            car_send, car_buf.at[k], car_ssem.at[k], car_rsem.at[k], {"sp": lax.rem(s + k, n)}
        )
        copy.start()
        carries.append(copy)
    for k in range(2, n):
        forward(k)
        for stage in range(stages - 1):
            arrived(k - 2, stage)
    for copy in carries:
        copy.wait()
    carry = jnp.zeros((1, gain_buf.shape[1]), jnp.float32)
    for k in range(n - 1, 0, -1):
        carry = jnp.where(k <= s, car_buf[k, 0:1] * carry + car_buf[k, 1:2], carry)
    states = states_ref[...] + gain_buf[...] * carry
    states_ref[...] = states
    prev_ref[...] = jnp.concatenate([carry, states[:-1]], axis=0)
    for k in range(n - 2, n):
        for stage in range(stages - 1):
            arrived(k, stage)
    for k in range(n):
        arrived(k, stages - 1)
    for copy in first:
        copy.wait_send()
    for copy in pushed:
        copy.wait_send()


def dispatch(send, decay, driven):
    n, m = lax.axis_size("sp"), lax.axis_size("tp")
    two, _, cap, feat = send.shape
    rows, channels = decay.shape
    vmem = pl.BlockSpec(memory_space=pltpu.VMEM)
    state = jax.ShapeDtypeStruct((rows, channels), jnp.float32)
    return pl.pallas_call(
        functools.partial(dispatch_kernel, n, m),
        out_shape=(jax.ShapeDtypeStruct((two, n, cap, m * feat), send.dtype), state, state),
        in_specs=[vmem] * 3,
        out_specs=(vmem,) * 3,
        scratch_shapes=[
            pltpu.VMEM((rows, channels), jnp.float32),
            pltpu.VMEM((2, channels), jnp.float32),
            pltpu.VMEM((n, 2, channels), jnp.float32),
            pltpu.SemaphoreType.DMA((n,)),
            pltpu.SemaphoreType.DMA((n,)),
            pltpu.SemaphoreType.DMA((m - 1, n)),
            pltpu.SemaphoreType.DMA((m - 1, n)),
            pltpu.SemaphoreType.DMA((n,)),
            pltpu.SemaphoreType.DMA((n,)),
            pltpu.SemaphoreType.DMA,
        ],
        compiler_params=pltpu.CompilerParams(collective_id=0, has_side_effects=True),
        name="dispatch",
    )(send, decay, driven)


def tail_kernel(
    n,
    decay_ref,
    input_ref,
    part_ref,
    grad_ref,
    sum_ref,
    gain_buf,
    car_send,
    car_buf,
    part_buf,
    part_ssem,
    part_rsem,
    car_ssem,
    car_rsem,
):
    s = lax.axis_index("sp")
    greet([{"sp": lax.rem(s + k, n)} for k in range(1, n)])
    parts = []
    for k in range(1, n):
        dst = lax.rem(s + k, n)
        copy = remote(
            part_ref.at[dst], part_buf.at[k], part_ssem.at[k], part_rsem.at[k], {"sp": dst}
        )
        parts.append(copy)
    decay = decay_ref[...]
    gain, term = local_scan(shifted(decay, 1, 1.0, True), input_ref[...], True)
    gain_buf[...] = gain
    grad_ref[...] = term
    car_send[0:1] = decay[0:1] * gain[0:1]
    car_send[1:2] = decay[0:1] * term[0:1]
    carries = []
    for k in range(1, n):
        copy = remote(
            car_send, car_buf.at[k], car_ssem.at[k], car_rsem.at[k], {"sp": lax.rem(s + k, n)}
        )
        copy.start()
        carries.append(copy)
    for copy in parts:
        copy.start()
    for copy in carries:
        copy.wait()
    carry = jnp.zeros((1, gain_buf.shape[1]), jnp.float32)
    for k in range(1, n):
        carry = jnp.where(k > s, car_buf[k, 0:1] * carry + car_buf[k, 1:2], carry)
    grad_ref[...] = grad_ref[...] + gain_buf[...] * carry
    sum_ref[...] = part_ref[s].astype(jnp.float32)
    for k in range(1, n):
        parts[k - 1].wait()
        sum_ref[...] += part_buf[k].astype(jnp.float32)


def tail(decay, state_in, part):
    n = lax.axis_size("sp")
    rows, channels = decay.shape
    vmem = pl.BlockSpec(memory_space=pltpu.VMEM)
    return pl.pallas_call(
        functools.partial(tail_kernel, n),
        out_shape=(
            jax.ShapeDtypeStruct((rows, channels), jnp.float32),
            jax.ShapeDtypeStruct(part.shape[1:], jnp.float32),
        ),
        in_specs=[vmem] * 3,
        out_specs=(vmem,) * 2,
        scratch_shapes=[
            pltpu.VMEM((rows, channels), jnp.float32),
            pltpu.VMEM((2, channels), jnp.float32),
            pltpu.VMEM((n, 2, channels), jnp.float32),
            pltpu.VMEM(part.shape, part.dtype),
            pltpu.SemaphoreType.DMA((n,)),
            pltpu.SemaphoreType.DMA((n,)),
            pltpu.SemaphoreType.DMA((n,)),
            pltpu.SemaphoreType.DMA((n,)),
        ],
        compiler_params=pltpu.CompilerParams(collective_id=1, has_side_effects=True),
        name="tail",
    )(decay, state_in, part)


def gelu_parts(output_gate_logits):
    gate_float = output_gate_logits.astype(jnp.float32)
    return jax.jvp(jax.nn.gelu, (gate_float,), (jnp.ones_like(gate_float),))


def expert_backward(inputs, cotangent, gate_weight, up_weight, down_weight):
    gate_act = jnp.dot(inputs, gate_weight, preferred_element_type=jnp.float32)
    up_act = jnp.dot(inputs, up_weight, preferred_element_type=jnp.float32)
    sigmoid_gate = jax.nn.sigmoid(gate_act)
    silu_act = gate_act * sigmoid_gate
    hidden = (silu_act * up_act).astype(jnp.bfloat16)
    d_hidden = lax.dot_general(
        cotangent, down_weight, (((1,), (1,)), ((), ())), preferred_element_type=jnp.float32
    )
    grad_down = lax.dot_general(
        hidden, cotangent, (((0,), (0,)), ((), ())), preferred_element_type=jnp.float32
    )
    d_gate = (d_hidden * up_act * sigmoid_gate * (1.0 + gate_act * (1.0 - sigmoid_gate))).astype(
        jnp.bfloat16
    )
    d_up = (d_hidden * silu_act).astype(jnp.bfloat16)
    grad_gate = lax.dot_general(
        inputs, d_gate, (((0,), (0,)), ((), ())), preferred_element_type=jnp.float32
    )
    grad_up = lax.dot_general(
        inputs, d_up, (((0,), (0,)), ((), ())), preferred_element_type=jnp.float32
    )
    partial_value = lax.dot_general(
        d_gate, gate_weight, (((1,), (1,)), ((), ())), preferred_element_type=jnp.float32
    )
    partial_value = partial_value + lax.dot_general(
        d_up, up_weight, (((1,), (1,)), ((), ())), preferred_element_type=jnp.float32
    )
    return (
        grad_gate.astype(jnp.bfloat16),
        grad_up.astype(jnp.bfloat16),
        grad_down.astype(jnp.bfloat16),
        partial_value,
    )


def per_device(
    middle_stream,
    output_gradient,
    routes,
    chosen_expert_weight,
    expert_gate_weight,
    expert_up_weight,
    expert_down_weight,
    recurrent_output_weight,
    recurrence_input,
    output_gate_logits,
    recurrence_gate_weight,
    input_gate_weight,
    channel_decay_param,
    extra_log_decay,
):
    rows_dev = middle_stream.shape[0]
    top_count = routes.shape[1]
    experts = lax.axis_size("sp")
    capacity = 3 * top_count * rows_dev // (2 * experts)
    feat_width = middle_stream.shape[1]
    choice = routes.T
    expert_ids = jnp.arange(experts, dtype=jnp.int32)
    named = [(choice[k][None, :] == expert_ids[:, None]) for k in range(top_count)]
    named_any = sum(part.astype(jnp.bfloat16) for part in named)
    position = jnp.arange(rows_dev, dtype=jnp.int32)
    earlier = (position[:, None] < position[None, :]).astype(jnp.bfloat16)
    rank = jnp.dot(named_any, earlier, preferred_element_type=jnp.float32).astype(jnp.int32)
    slot_ids = jnp.arange(experts * capacity, dtype=jnp.int32)
    picks = []
    for k in range(top_count):
        slot = jnp.sum(
            jnp.where(named[k], rank + expert_ids[:, None] * capacity, 0), axis=0, keepdims=True
        )
        picks.append((slot_ids[:, None] == slot).astype(jnp.bfloat16))
    pick_any = sum(picks)
    pick_both = jnp.concatenate(picks, axis=1)
    pair_cot = (
        chosen_expert_weight.T[:, :, None] * output_gradient.astype(jnp.float32)[None]
    ).astype(jnp.bfloat16)
    pair_cot = pair_cot.reshape(-1, feat_width)
    send_rows = jnp.dot(pick_any, middle_stream, preferred_element_type=jnp.bfloat16)
    send_cot = jnp.dot(pick_both, pair_cot, preferred_element_type=jnp.bfloat16)
    send = jnp.stack([send_rows, send_cot]).reshape(2, experts, capacity, feat_width)
    channels = recurrence_input.shape[1]
    block_width = recurrence_gate_weight.shape[1]
    local_blocks = channels // block_width
    first_block = lax.axis_index("tp") * local_blocks
    recall_weight = lax.dynamic_slice_in_dim(recurrence_gate_weight, first_block, local_blocks, 0)
    admit_weight = lax.dynamic_slice_in_dim(input_gate_weight, first_block, local_blocks, 0)
    u_blocks = recurrence_input.reshape(rows_dev, local_blocks, block_width)
    forget_gate = jax.nn.sigmoid(
        jnp.einsum(
            "tnb,nbc->tnc", u_blocks, recall_weight, preferred_element_type=jnp.float32
        ).reshape(rows_dev, channels)
    )
    admit_gate = jax.nn.sigmoid(
        jnp.einsum(
            "tnb,nbc->tnc", u_blocks, admit_weight, preferred_element_type=jnp.float32
        ).reshape(rows_dev, channels)
    )
    baseline_rate = jax.nn.softplus(-channel_decay_param)
    decay_logarithm = -8.0 * forget_gate * baseline_rate[None, :] + extra_log_decay
    decay_step = jnp.exp(decay_logarithm)
    input_scale = jnp.sqrt(-jnp.expm1(2.0 * decay_logarithm))
    u_float = recurrence_input.astype(jnp.float32)
    driven = u_float * admit_gate * input_scale
    received, states, prev_states = dispatch(send, decay_step, driven)
    row_width = received.shape[3]
    inputs = received[0].reshape(-1, row_width)
    cotangent = received[1].reshape(-1, row_width)
    grad_gate, grad_up, grad_down, partial_value = expert_backward(
        inputs, cotangent, expert_gate_weight[0], expert_up_weight[0], expert_down_weight[0]
    )
    slot_grad = lax.psum_scatter(
        partial_value.astype(jnp.bfloat16), "tp", scatter_dimension=1, tiled=True
    )
    returned = lax.all_to_all(slot_grad[None], "sp", split_axis=1, concat_axis=0, tiled=True)
    arrived = lax.dot_general(
        pick_any,
        returned.reshape(experts * capacity, -1),
        (((0,), (0,)), ((), ())),
        preferred_element_type=jnp.float32,
    )
    residual_grad = (output_gradient.astype(jnp.float32) + arrived).astype(jnp.bfloat16)
    grad_full = lax.all_gather(residual_grad, "tp", axis=1, tiled=True)
    mixer_grad = jnp.dot(grad_full, recurrent_output_weight, preferred_element_type=jnp.float32)
    gelu_val, gelu_der = gelu_parts(output_gate_logits)
    lru_out = (states * gelu_val).astype(jnp.bfloat16)
    gop_part = lax.dot_general(
        grad_full, lru_out, (((0,), (0,)), ((), ())), preferred_element_type=jnp.float32
    ).astype(jnp.bfloat16)
    gop_part = gop_part.reshape(experts, -1, channels)
    grad_gate_pre = mixer_grad * states * gelu_der
    state_in = mixer_grad * gelu_val
    state_grad, grad_out_proj = tail(decay_step, state_in, gop_part)
    d_log = state_grad * (
        prev_states * decay_step - u_float * admit_gate * decay_step * decay_step / input_scale
    )
    d_recall = (d_log * (-8.0 * baseline_rate[None, :]) * forget_gate * (1.0 - forget_gate)).astype(
        jnp.bfloat16
    )
    d_admit = (state_grad * u_float * input_scale * admit_gate * (1.0 - admit_gate)).astype(
        jnp.bfloat16
    )
    back_recall = jnp.einsum(
        "tnc,nbc->tnb",
        d_recall.reshape(rows_dev, local_blocks, block_width),
        recall_weight,
        preferred_element_type=jnp.float32,
    )
    back_admit = jnp.einsum(
        "tnc,nbc->tnb",
        d_admit.reshape(rows_dev, local_blocks, block_width),
        admit_weight,
        preferred_element_type=jnp.float32,
    )
    grad_input = state_grad * admit_gate * input_scale + (back_recall + back_admit).reshape(
        rows_dev, channels
    )
    return (
        grad_gate[None],
        grad_up[None],
        grad_down[None],
        grad_out_proj,
        grad_input,
        grad_gate_pre,
    )


def solution(mesh):
    placed = (
        P("sp", "tp"),
        P("sp", "tp"),
        P("sp", None),
        P("sp", None),
        P("sp", None, "tp"),
        P("sp", None, "tp"),
        P("sp", "tp", None),
        P(None, "tp"),
        P("sp", "tp"),
        P("sp", "tp"),
        P(),
        P(),
        P("tp"),
        P("sp", "tp"),
    )
    return jax.shard_map(
        per_device,
        mesh=mesh,
        in_specs=placed,
        out_specs=(
            P("sp", None, "tp"),
            P("sp", None, "tp"),
            P("sp", "tp", None),
            P("sp", "tp"),
            P("sp", "tp"),
            P("sp", "tp"),
        ),
        check_vma=False,
    )
```

```python
import functools

import jax
import jax.numpy as jnp
from jax import lax
from jax.experimental import pallas as pl
from jax.experimental.pallas import tpu as pltpu
from jax.sharding import PartitionSpec as P

MESH = pl.DeviceIdType.MESH


def partner(t, stage, m):
    d = m >> (stage + 1)
    return t + d * (1 - 2 * ((t // d) % 2))


def held_columns(t, stage, m):
    if stage == 0:
        return [t]
    return held_columns(t, stage - 1, m) + held_columns(partner(t, stage - 1, m), stage - 1, m)


def greet(peers):
    barrier = pltpu.get_barrier_semaphore()
    for peer in peers:
        pl.semaphore_signal(barrier, inc=1, device_id=peer, device_id_type=MESH)
    pl.semaphore_wait(barrier, len(peers))


def remote(src, dst, send_sem, recv_sem, peer):
    return pltpu.make_async_remote_copy(
        src_ref=src,
        dst_ref=dst,
        send_sem=send_sem,
        recv_sem=recv_sem,
        device_id=peer,
        device_id_type=MESH,
    )


def shifted(value, k, fill, reverse):
    pad = jnp.full((k, value.shape[1]), fill, value.dtype)
    if reverse:
        return jnp.concatenate([value[k:], pad], axis=0)
    return jnp.concatenate([pad, value[:-k]], axis=0)


def local_scan(gain, term, reverse):
    k = 1
    while k < gain.shape[0]:
        term = term + gain * shifted(term, k, 0.0, reverse)
        gain = gain * shifted(gain, k, 1.0, reverse)
        k *= 2
    return gain, term


def dispatch_kernel(
    n,
    m,
    rows_ref,
    cot_ref,
    decay_ref,
    driven_ref,
    rows_out,
    cot_out,
    states_ref,
    prev_ref,
    gain_buf,
    car_send,
    car_buf,
    a2a_send,
    a2a_recv,
    tp_send,
    tp_recv,
    car_ssem,
    car_rsem,
    self_sem,
):
    sources, targets = (rows_ref, cot_ref), (rows_out, cot_out)
    s, t = lax.axis_index("sp"), lax.axis_index("tp")
    feat = rows_ref.shape[2]
    stages = m.bit_length() - 1
    greet(
        [{"sp": lax.rem(s + k, n)} for k in range(1, n)]
        + [{"tp": partner(t, j, m)} for j in range(stages)]
    )

    def block(a, src, col):
        return targets[a].at[src, :, pl.ds(pl.multiple_of(col * feat, feat), feat)]

    first = []
    for k in range(n):
        dst = lax.rem(s + k, n)
        for a in range(2):
            if k == 0:
                copy = pltpu.make_async_copy(sources[a].at[s], block(a, s, t), self_sem.at[a])
            else:
                copy = remote(
                    sources[a].at[dst],
                    block(a, s, t),
                    a2a_send.at[a, k],
                    a2a_recv.at[a, k],
                    {"sp": dst},
                )
            copy.start()
            first.append(copy)

    pushed = []

    def push(a, k, stage, i, col):
        src = lax.rem(s + n - k, n)
        at = 2**stage - 1 + i
        copy = remote(
            block(a, src, col),
            block(a, src, col),
            tp_send.at[a, at, k],
            tp_recv.at[a, at, k],
            {"tp": partner(t, stage, m)},
        )
        copy.start()
        pushed.append(copy)

    def arrived(k, stage):
        src = lax.rem(s + n - k, n)
        cols = held_columns(partner(t, stage, m), stage, m)
        for i, col in enumerate(cols):
            at = 2**stage - 1 + i
            for a in range(2):
                remote(
                    block(a, src, col),
                    block(a, src, col),
                    tp_send.at[a, at, k],
                    tp_recv.at[a, at, k],
                    {"tp": partner(t, stage, m)},
                ).wait_recv()
                for later in range(stage + 1, stages):
                    push(a, k, later, 2**stage + i, col)

    def forward(k):
        for a in range(2):
            if k == 0:
                first[a].wait()
            else:
                first[2 * k + a].wait_recv()
            for stage in range(stages):
                push(a, k, stage, 0, t)

    forward(0)
    gain, term = local_scan(decay_ref[...], driven_ref[...], False)
    gain_buf[...] = gain
    states_ref[...] = term
    rows = gain.shape[0]
    car_send[0:1] = gain[rows - 1 : rows]
    car_send[1:2] = term[rows - 1 : rows]
    forward(1)
    carries = []
    for k in range(1, n):
        copy = remote(
            car_send, car_buf.at[k], car_ssem.at[k], car_rsem.at[k], {"sp": lax.rem(s + k, n)}
        )
        copy.start()
        carries.append(copy)
    for k in range(2, n):
        forward(k)
        for stage in range(stages - 1):
            arrived(k - 2, stage)
    for copy in carries:
        copy.wait()
    carry = jnp.zeros((1, gain_buf.shape[1]), jnp.float32)
    for k in range(n - 1, 0, -1):
        carry = jnp.where(k <= s, car_buf[k, 0:1] * carry + car_buf[k, 1:2], carry)
    states = states_ref[...] + gain_buf[...] * carry
    states_ref[...] = states
    prev_ref[...] = jnp.concatenate([carry, states[:-1]], axis=0)
    for k in range(n - 2, n):
        for stage in range(stages - 1):
            arrived(k, stage)
    for k in range(n):
        arrived(k, stages - 1)
    for copy in first[2:]:
        copy.wait_send()
    for copy in pushed:
        copy.wait_send()


def dispatch(send_rows, send_cot, decay, driven):
    n, m = lax.axis_size("sp"), lax.axis_size("tp")
    _, cap, feat = send_rows.shape
    whole = jax.ShapeDtypeStruct((n, cap, m * feat), send_rows.dtype)
    rows, channels = decay.shape
    vmem = pl.BlockSpec(memory_space=pltpu.VMEM)
    state = jax.ShapeDtypeStruct((rows, channels), jnp.float32)
    return pl.pallas_call(
        functools.partial(dispatch_kernel, n, m),
        out_shape=(whole, whole, state, state),
        in_specs=[vmem] * 4,
        out_specs=(vmem,) * 4,
        scratch_shapes=[
            pltpu.VMEM((rows, channels), jnp.float32),
            pltpu.VMEM((2, channels), jnp.float32),
            pltpu.VMEM((n, 2, channels), jnp.float32),
            pltpu.SemaphoreType.DMA((2, n)),
            pltpu.SemaphoreType.DMA((2, n)),
            pltpu.SemaphoreType.DMA((2, m - 1, n)),
            pltpu.SemaphoreType.DMA((2, m - 1, n)),
            pltpu.SemaphoreType.DMA((n,)),
            pltpu.SemaphoreType.DMA((n,)),
            pltpu.SemaphoreType.DMA((2,)),
        ],
        compiler_params=pltpu.CompilerParams(collective_id=0, has_side_effects=True),
        name="dispatch",
    )(send_rows, send_cot, decay, driven)


def return_kernel(
    n,
    m,
    part_ref,
    pick_ref,
    cot_ref,
    out_ref,
    in_buf,
    acc_buf,
    back_buf,
    rs_send,
    rs_recv,
    a2a_send,
    a2a_recv,
    ag_send,
    ag_recv,
):
    s, t = lax.axis_index("sp"), lax.axis_index("tp")
    feat = cot_ref.shape[1]
    stages = m.bit_length() - 1

    def across(stage):
        d = 2**stage
        return t + d * (1 - 2 * ((t // d) % 2))

    greet(
        [{"sp": lax.rem(s + k, n)} for k in range(1, n)] + [{"tp": across(j)} for j in range(stages)]
    )

    def cols(col):
        return pl.ds(pl.multiple_of(col * feat, feat), feat)

    base = []
    total = 0
    for stage in range(stages):
        base.append(total)
        total += m >> (stage + 1)

    order = list(range(1, n)) + [0]
    waits = []

    def send_stage(k, stage):
        dst = lax.rem(s + k, n)
        source = part_ref if stage == 0 else acc_buf
        peer = across(stage)
        step = 2 ** (stage + 1)
        for i in range(m // step):
            col = lax.rem(peer + i * step, m)
            at = base[stage] + i
            copy = remote(
                source.at[dst, :, cols(col)],
                in_buf.at[at, k],
                rs_send.at[at, k],
                rs_recv.at[at, k],
                {"tp": peer},
            )
            copy.start()
            waits.append(copy)

    def sum_stage(k, stage):
        dst = lax.rem(s + k, n)
        source = part_ref if stage == 0 else acc_buf
        step = 2 ** (stage + 1)
        for i in range(m // step):
            col = lax.rem(t + i * step, m)
            at = base[stage] + i
            remote(
                source.at[dst, :, cols(col)],
                in_buf.at[at, k],
                rs_send.at[at, k],
                rs_recv.at[at, k],
                {"tp": across(stage)},
            ).wait_recv()
            mine = source[dst, :, cols(col)].astype(jnp.float32)
            acc_buf[dst, :, cols(col)] = (mine + in_buf[at, k].astype(jnp.float32)).astype(
                jnp.bfloat16
            )

    def send_home(k):
        dst = lax.rem(s + k, n)
        if k == 0:
            back_buf[s] = acc_buf[s, :, cols(t)]
            return
        copy = remote(
            acc_buf.at[dst, :, cols(t)],
            back_buf.at[s],
            a2a_send.at[k],
            a2a_recv.at[k],
            {"sp": dst},
        )
        copy.start()
        waits.append(copy)

    for k in order:
        send_stage(k, 0)
    for at in range(n + stages - 1):
        for stage in range(stages):
            if 0 <= at - stage < n:
                k = order[at - stage]
                sum_stage(k, stage)
                if stage + 1 < stages:
                    send_stage(k, stage + 1)
                else:
                    send_home(k)
    value = cot_ref[...].astype(jnp.float32)
    for k in range(n):
        src = lax.rem(s + n - k, n)
        if k > 0:
            remote(
                acc_buf.at[src, :, cols(t)],
                back_buf.at[src],
                a2a_send.at[k],
                a2a_recv.at[k],
                {"sp": src},
            ).wait_recv()
        value = value + jnp.dot(
            pick_ref[src], back_buf[src], preferred_element_type=jnp.float32
        )
    out_ref[:, cols(t)] = value.astype(jnp.bfloat16)

    def share(stage, i, col):
        at = 2**stage - 1 + i
        return remote(
            out_ref.at[:, cols(col)],
            out_ref.at[:, cols(col)],
            ag_send.at[at],
            ag_recv.at[at],
            {"tp": partner(t, stage, m)},
        )

    def push(stage, i, col):
        copy = share(stage, i, col)
        copy.start()
        waits.append(copy)

    for stage in range(stages):
        push(stage, 0, t)
    for stage in range(stages):
        for i, col in enumerate(held_columns(partner(t, stage, m), stage, m)):
            share(stage, i, col).wait_recv()
            for later in range(stage + 1, stages):
                push(later, 2**stage + i, col)
    for copy in waits:
        copy.wait_send()


def bring_back(part, pick, output_gradient):
    n, m = lax.axis_size("sp"), lax.axis_size("tp")
    _, cap, width = part.shape
    rows, feat = output_gradient.shape
    vmem = pl.BlockSpec(memory_space=pltpu.VMEM)
    return pl.pallas_call(
        functools.partial(return_kernel, n, m),
        out_shape=jax.ShapeDtypeStruct((rows, width), jnp.bfloat16),
        in_specs=[vmem] * 3,
        out_specs=vmem,
        scratch_shapes=[
            pltpu.VMEM((m - 1, n, cap, feat), jnp.bfloat16),
            pltpu.VMEM((n, cap, width), jnp.bfloat16),
            pltpu.VMEM((n, cap, feat), jnp.bfloat16),
            pltpu.SemaphoreType.DMA((m - 1, n)),
            pltpu.SemaphoreType.DMA((m - 1, n)),
            pltpu.SemaphoreType.DMA((n,)),
            pltpu.SemaphoreType.DMA((n,)),
            pltpu.SemaphoreType.DMA((m - 1,)),
            pltpu.SemaphoreType.DMA((m - 1,)),
        ],
        compiler_params=pltpu.CompilerParams(collective_id=2, has_side_effects=True),
        name="bring_back",
    )(part, pick, output_gradient)


def tail_kernel(
    n,
    decay_ref,
    input_ref,
    part_ref,
    grad_ref,
    sum_ref,
    gain_buf,
    car_send,
    car_buf,
    part_buf,
    part_ssem,
    part_rsem,
    car_ssem,
    car_rsem,
):
    s = lax.axis_index("sp")
    greet([{"sp": lax.rem(s + k, n)} for k in range(1, n)])
    parts = []
    for k in range(1, n):
        dst = lax.rem(s + k, n)
        copy = remote(
            part_ref.at[dst], part_buf.at[k], part_ssem.at[k], part_rsem.at[k], {"sp": dst}
        )
        parts.append(copy)
    decay = decay_ref[...]
    gain, term = local_scan(shifted(decay, 1, 1.0, True), input_ref[...], True)
    gain_buf[...] = gain
    grad_ref[...] = term
    car_send[0:1] = decay[0:1] * gain[0:1]
    car_send[1:2] = decay[0:1] * term[0:1]
    carries = []
    for k in range(1, n):
        copy = remote(
            car_send, car_buf.at[k], car_ssem.at[k], car_rsem.at[k], {"sp": lax.rem(s + k, n)}
        )
        copy.start()
        carries.append(copy)
    for copy in parts:
        copy.start()
    for copy in carries:
        copy.wait()
    carry = jnp.zeros((1, gain_buf.shape[1]), jnp.float32)
    for k in range(1, n):
        carry = jnp.where(k > s, car_buf[k, 0:1] * carry + car_buf[k, 1:2], carry)
    grad_ref[...] = grad_ref[...] + gain_buf[...] * carry
    sum_ref[...] = part_ref[s].astype(jnp.float32)
    for k in range(1, n):
        parts[k - 1].wait()
        sum_ref[...] += part_buf[k].astype(jnp.float32)


def tail(decay, state_in, part):
    n = lax.axis_size("sp")
    rows, channels = decay.shape
    vmem = pl.BlockSpec(memory_space=pltpu.VMEM)
    return pl.pallas_call(
        functools.partial(tail_kernel, n),
        out_shape=(
            jax.ShapeDtypeStruct((rows, channels), jnp.float32),
            jax.ShapeDtypeStruct(part.shape[1:], jnp.float32),
        ),
        in_specs=[vmem] * 3,
        out_specs=(vmem,) * 2,
        scratch_shapes=[
            pltpu.VMEM((rows, channels), jnp.float32),
            pltpu.VMEM((2, channels), jnp.float32),
            pltpu.VMEM((n, 2, channels), jnp.float32),
            pltpu.VMEM(part.shape, part.dtype),
            pltpu.SemaphoreType.DMA((n,)),
            pltpu.SemaphoreType.DMA((n,)),
            pltpu.SemaphoreType.DMA((n,)),
            pltpu.SemaphoreType.DMA((n,)),
        ],
        compiler_params=pltpu.CompilerParams(collective_id=1, has_side_effects=True),
        name="tail",
    )(decay, state_in, part)


def gelu_parts(output_gate_logits):
    gate_float = output_gate_logits.astype(jnp.float32)
    return jax.jvp(jax.nn.gelu, (gate_float,), (jnp.ones_like(gate_float),))


def expert_backward(inputs, cotangent, gate_weight, up_weight, down_weight):
    gate_act = jnp.dot(inputs, gate_weight, preferred_element_type=jnp.float32)
    up_act = jnp.dot(inputs, up_weight, preferred_element_type=jnp.float32)
    sigmoid_gate = jax.nn.sigmoid(gate_act)
    silu_act = gate_act * sigmoid_gate
    hidden = (silu_act * up_act).astype(jnp.bfloat16)
    d_hidden = lax.dot_general(
        cotangent, down_weight, (((1,), (1,)), ((), ())), preferred_element_type=jnp.float32
    )
    grad_down = lax.dot_general(
        hidden, cotangent, (((0,), (0,)), ((), ())), preferred_element_type=jnp.float32
    )
    d_gate = (d_hidden * up_act * sigmoid_gate * (1.0 + gate_act * (1.0 - sigmoid_gate))).astype(
        jnp.bfloat16
    )
    d_up = (d_hidden * silu_act).astype(jnp.bfloat16)
    grad_gate = lax.dot_general(
        inputs, d_gate, (((0,), (0,)), ((), ())), preferred_element_type=jnp.float32
    )
    grad_up = lax.dot_general(
        inputs, d_up, (((0,), (0,)), ((), ())), preferred_element_type=jnp.float32
    )
    partial_value = lax.dot_general(
        d_gate, gate_weight, (((1,), (1,)), ((), ())), preferred_element_type=jnp.float32
    )
    partial_value = partial_value + lax.dot_general(
        d_up, up_weight, (((1,), (1,)), ((), ())), preferred_element_type=jnp.float32
    )
    return (
        grad_gate.astype(jnp.bfloat16),
        grad_up.astype(jnp.bfloat16),
        grad_down.astype(jnp.bfloat16),
        partial_value,
    )


def per_device(
    middle_stream,
    output_gradient,
    routes,
    chosen_expert_weight,
    expert_gate_weight,
    expert_up_weight,
    expert_down_weight,
    recurrent_output_weight,
    recurrence_input,
    output_gate_logits,
    recurrence_gate_weight,
    input_gate_weight,
    channel_decay_param,
    extra_log_decay,
):
    rows_dev = middle_stream.shape[0]
    top_count = routes.shape[1]
    experts = lax.axis_size("sp")
    capacity = 3 * top_count * rows_dev // (2 * experts)
    feat_width = middle_stream.shape[1]
    choice = routes.T
    expert_ids = jnp.arange(experts, dtype=jnp.int32)
    named = [(choice[k][None, :] == expert_ids[:, None]) for k in range(top_count)]
    named_any = sum(part.astype(jnp.bfloat16) for part in named)
    position = jnp.arange(rows_dev, dtype=jnp.int32)
    earlier = (position[:, None] < position[None, :]).astype(jnp.bfloat16)
    rank = jnp.dot(named_any, earlier, preferred_element_type=jnp.float32).astype(jnp.int32)
    slot_ids = jnp.arange(experts * capacity, dtype=jnp.int32)
    picks = []
    for k in range(top_count):
        slot = jnp.sum(
            jnp.where(named[k], rank + expert_ids[:, None] * capacity, 0), axis=0, keepdims=True
        )
        picks.append((slot_ids[:, None] == slot).astype(jnp.bfloat16))
    pick_any = sum(picks)
    pick_both = jnp.concatenate(picks, axis=1)
    pair_cot = (
        chosen_expert_weight.T[:, :, None] * output_gradient.astype(jnp.float32)[None]
    ).astype(jnp.bfloat16)
    pair_cot = pair_cot.reshape(-1, feat_width)
    send_rows = jnp.dot(pick_any, middle_stream, preferred_element_type=jnp.bfloat16)
    send_cot = jnp.dot(pick_both, pair_cot, preferred_element_type=jnp.bfloat16)
    channels = recurrence_input.shape[1]
    block_width = recurrence_gate_weight.shape[1]
    local_blocks = channels // block_width
    first_block = lax.axis_index("tp") * local_blocks
    recall_weight = lax.dynamic_slice_in_dim(recurrence_gate_weight, first_block, local_blocks, 0)
    admit_weight = lax.dynamic_slice_in_dim(input_gate_weight, first_block, local_blocks, 0)
    u_blocks = recurrence_input.reshape(rows_dev, local_blocks, block_width)
    forget_gate = jax.nn.sigmoid(
        jnp.einsum(
            "tnb,nbc->tnc", u_blocks, recall_weight, preferred_element_type=jnp.float32
        ).reshape(rows_dev, channels)
    )
    admit_gate = jax.nn.sigmoid(
        jnp.einsum(
            "tnb,nbc->tnc", u_blocks, admit_weight, preferred_element_type=jnp.float32
        ).reshape(rows_dev, channels)
    )
    baseline_rate = jax.nn.softplus(-channel_decay_param)
    decay_logarithm = -8.0 * forget_gate * baseline_rate[None, :] + extra_log_decay
    decay_step = jnp.exp(decay_logarithm)
    input_scale = jnp.sqrt(-jnp.expm1(2.0 * decay_logarithm))
    u_float = recurrence_input.astype(jnp.float32)
    driven = u_float * admit_gate * input_scale
    recv_rows, recv_cot, states, prev_states = dispatch(
        send_rows.reshape(experts, capacity, feat_width),
        send_cot.reshape(experts, capacity, feat_width),
        decay_step,
        driven,
    )
    row_width = recv_rows.shape[2]
    inputs = recv_rows.reshape(-1, row_width)
    cotangent = recv_cot.reshape(-1, row_width)
    grad_gate, grad_up, grad_down, partial_value = expert_backward(
        inputs, cotangent, expert_gate_weight[0], expert_up_weight[0], expert_down_weight[0]
    )
    grad_full = bring_back(
        partial_value.astype(jnp.bfloat16).reshape(experts, capacity, row_width),
        pick_any.reshape(experts, capacity, rows_dev).transpose(0, 2, 1),
        output_gradient,
    )
    mixer_grad = jnp.dot(grad_full, recurrent_output_weight, preferred_element_type=jnp.float32)
    gelu_val, gelu_der = gelu_parts(output_gate_logits)
    lru_out = (states * gelu_val).astype(jnp.bfloat16)
    gop_part = lax.dot_general(
        grad_full, lru_out, (((0,), (0,)), ((), ())), preferred_element_type=jnp.float32
    ).astype(jnp.bfloat16)
    gop_part = gop_part.reshape(experts, -1, channels)
    grad_gate_pre = mixer_grad * states * gelu_der
    state_in = mixer_grad * gelu_val
    state_grad, grad_out_proj = tail(decay_step, state_in, gop_part)
    d_log = state_grad * (
        prev_states * decay_step - u_float * admit_gate * decay_step * decay_step / input_scale
    )
    d_recall = (d_log * (-8.0 * baseline_rate[None, :]) * forget_gate * (1.0 - forget_gate)).astype(
        jnp.bfloat16
    )
    d_admit = (state_grad * u_float * input_scale * admit_gate * (1.0 - admit_gate)).astype(
        jnp.bfloat16
    )
    back_recall = jnp.einsum(
        "tnc,nbc->tnb",
        d_recall.reshape(rows_dev, local_blocks, block_width),
        recall_weight,
        preferred_element_type=jnp.float32,
    )
    back_admit = jnp.einsum(
        "tnc,nbc->tnb",
        d_admit.reshape(rows_dev, local_blocks, block_width),
        admit_weight,
        preferred_element_type=jnp.float32,
    )
    grad_input = state_grad * admit_gate * input_scale + (back_recall + back_admit).reshape(
        rows_dev, channels
    )
    return (
        grad_gate[None],
        grad_up[None],
        grad_down[None],
        grad_out_proj,
        grad_input,
        grad_gate_pre,
    )


def solution(mesh):
    placed = (
        P("sp", "tp"),
        P("sp", "tp"),
        P("sp", None),
        P("sp", None),
        P("sp", None, "tp"),
        P("sp", None, "tp"),
        P("sp", "tp", None),
        P(None, "tp"),
        P("sp", "tp"),
        P("sp", "tp"),
        P(),
        P(),
        P("tp"),
        P("sp", "tp"),
    )
    return jax.shard_map(
        per_device,
        mesh=mesh,
        in_specs=placed,
        out_specs=(
            P("sp", None, "tp"),
            P("sp", None, "tp"),
            P("sp", "tp", None),
            P("sp", "tp"),
            P("sp", "tp"),
            P("sp", "tp"),
        ),
        check_vma=False,
    )
```

```python
import functools

import jax
import jax.numpy as jnp
from jax import lax
from jax.experimental import pallas as pl
from jax.experimental.pallas import tpu as pltpu
from jax.sharding import PartitionSpec as P

MESH = pl.DeviceIdType.MESH


def partner(t, stage, m):
    d = m >> (stage + 1)
    return t + d * (1 - 2 * ((t // d) % 2))


def flipped(s, j, n):
    out = 0
    for b in range(n.bit_length() - 1):
        bit = (s // 2**b) % 2
        out = out + (1 - bit if (j >> b) % 2 else bit) * 2**b
    return out


def far_near(n):
    near, far = list(range(n // 2)), list(range(n // 2, n))
    arrive = near[:1]
    for i in range(1, n // 2):
        arrive += [near[i], far[i - 1]]
    leave = []
    for i in range(1, n // 2):
        leave += [far[i - 1], near[i]]
    return arrive + far[-1:], leave + far[-1:], far + near[1:] + near[:1]


def held_columns(t, stage, m):
    if stage == 0:
        return [t]
    return held_columns(t, stage - 1, m) + held_columns(partner(t, stage - 1, m), stage - 1, m)


def greet(peers):
    barrier = pltpu.get_barrier_semaphore()
    for peer in peers:
        pl.semaphore_signal(barrier, inc=1, device_id=peer, device_id_type=MESH)
    pl.semaphore_wait(barrier, len(peers))


def remote(src, dst, send_sem, recv_sem, peer):
    return pltpu.make_async_remote_copy(
        src_ref=src,
        dst_ref=dst,
        send_sem=send_sem,
        recv_sem=recv_sem,
        device_id=peer,
        device_id_type=MESH,
    )


def shifted(value, k, fill, reverse):
    pad = jnp.full((k, value.shape[1]), fill, value.dtype)
    if reverse:
        return jnp.concatenate([value[k:], pad], axis=0)
    return jnp.concatenate([pad, value[:-k]], axis=0)


def local_scan(gain, term, reverse):
    k = 1
    while k < gain.shape[0]:
        term = term + gain * shifted(term, k, 0.0, reverse)
        gain = gain * shifted(gain, k, 1.0, reverse)
        k *= 2
    return gain, term


def dispatch_kernel(
    n,
    m,
    rows_ref,
    cot_ref,
    decay_ref,
    driven_ref,
    rows_out,
    cot_out,
    states_ref,
    prev_ref,
    gain_buf,
    car_send,
    car_buf,
    a2a_send,
    a2a_recv,
    tp_send,
    tp_recv,
    car_ssem,
    car_rsem,
    self_sem,
):
    sources, targets = (rows_ref, cot_ref), (rows_out, cot_out)
    s, t = lax.axis_index("sp"), lax.axis_index("tp")
    feat = rows_ref.shape[2]
    stages = m.bit_length() - 1
    greet(
        [{"sp": lax.rem(s + k, n)} for k in range(1, n)]
        + [{"tp": partner(t, j, m)} for j in range(stages)]
    )

    def block(a, src, col):
        return targets[a].at[src, :, pl.ds(pl.multiple_of(col * feat, feat), feat)]

    first = {}
    arrive, leave, _ = far_near(n)
    for k in [0] + leave:
        dst = flipped(s, k, n)
        for a in range(2):
            if k == 0:
                copy = pltpu.make_async_copy(sources[a].at[s], block(a, s, t), self_sem.at[a])
            else:
                copy = remote(
                    sources[a].at[dst],
                    block(a, s, t),
                    a2a_send.at[a, k],
                    a2a_recv.at[a, k],
                    {"sp": dst},
                )
            copy.start()
            first[k, a] = copy

    pushed = []

    def push(a, k, stage, i, col):
        src = flipped(s, k, n)
        at = 2**stage - 1 + i
        copy = remote(
            block(a, src, col),
            block(a, src, col),
            tp_send.at[a, at, k],
            tp_recv.at[a, at, k],
            {"tp": partner(t, stage, m)},
        )
        copy.start()
        pushed.append(copy)

    def arrived(k, stage):
        src = flipped(s, k, n)
        cols = held_columns(partner(t, stage, m), stage, m)
        for i, col in enumerate(cols):
            at = 2**stage - 1 + i
            for a in range(2):
                remote(
                    block(a, src, col),
                    block(a, src, col),
                    tp_send.at[a, at, k],
                    tp_recv.at[a, at, k],
                    {"tp": partner(t, stage, m)},
                ).wait_recv()
                for later in range(stage + 1, stages):
                    push(a, k, later, 2**stage + i, col)

    def forward(k):
        for a in range(2):
            if k == 0:
                first[k, a].wait()
            else:
                first[k, a].wait_recv()
            for stage in range(stages):
                push(a, k, stage, 0, t)

    forward(arrive[0])
    gain, term = local_scan(decay_ref[...], driven_ref[...], False)
    gain_buf[...] = gain
    states_ref[...] = term
    rows = gain.shape[0]
    car_send[0:1] = gain[rows - 1 : rows]
    car_send[1:2] = term[rows - 1 : rows]
    forward(arrive[1])
    carries = []
    for k in range(1, n):
        copy = remote(
            car_send, car_buf.at[k], car_ssem.at[k], car_rsem.at[k], {"sp": lax.rem(s + k, n)}
        )
        copy.start()
        carries.append(copy)
    for at in range(2, n):
        forward(arrive[at])
        for stage in range(stages - 1):
            arrived(arrive[at - 2], stage)
    for copy in carries:
        copy.wait()
    carry = jnp.zeros((1, gain_buf.shape[1]), jnp.float32)
    for k in range(n - 1, 0, -1):
        carry = jnp.where(k <= s, car_buf[k, 0:1] * carry + car_buf[k, 1:2], carry)
    states = states_ref[...] + gain_buf[...] * carry
    states_ref[...] = states
    prev_ref[...] = jnp.concatenate([carry, states[:-1]], axis=0)
    for k in arrive[n - 2 :]:
        for stage in range(stages - 1):
            arrived(k, stage)
    for k in range(n):
        arrived(k, stages - 1)
    for k in leave:
        for a in range(2):
            first[k, a].wait_send()
    for copy in pushed:
        copy.wait_send()


def dispatch(send_rows, send_cot, decay, driven):
    n, m = lax.axis_size("sp"), lax.axis_size("tp")
    _, cap, feat = send_rows.shape
    whole = jax.ShapeDtypeStruct((n, cap, m * feat), send_rows.dtype)
    rows, channels = decay.shape
    vmem = pl.BlockSpec(memory_space=pltpu.VMEM)
    state = jax.ShapeDtypeStruct((rows, channels), jnp.float32)
    return pl.pallas_call(
        functools.partial(dispatch_kernel, n, m),
        out_shape=(whole, whole, state, state),
        in_specs=[vmem] * 4,
        out_specs=(vmem,) * 4,
        scratch_shapes=[
            pltpu.VMEM((rows, channels), jnp.float32),
            pltpu.VMEM((2, channels), jnp.float32),
            pltpu.VMEM((n, 2, channels), jnp.float32),
            pltpu.SemaphoreType.DMA((2, n)),
            pltpu.SemaphoreType.DMA((2, n)),
            pltpu.SemaphoreType.DMA((2, m - 1, n)),
            pltpu.SemaphoreType.DMA((2, m - 1, n)),
            pltpu.SemaphoreType.DMA((n,)),
            pltpu.SemaphoreType.DMA((n,)),
            pltpu.SemaphoreType.DMA((2,)),
        ],
        compiler_params=pltpu.CompilerParams(collective_id=0, has_side_effects=True),
        name="dispatch",
    )(send_rows, send_cot, decay, driven)


def return_kernel(
    n,
    m,
    part_ref,
    pick_ref,
    cot_ref,
    out_ref,
    in_buf,
    acc_buf,
    back_buf,
    rs_send,
    rs_recv,
    a2a_send,
    a2a_recv,
    ag_send,
    ag_recv,
):
    s, t = lax.axis_index("sp"), lax.axis_index("tp")
    feat = cot_ref.shape[1]
    stages = m.bit_length() - 1

    def across(stage):
        d = 2**stage
        return t + d * (1 - 2 * ((t // d) % 2))

    greet(
        [{"sp": lax.rem(s + k, n)} for k in range(1, n)] + [{"tp": across(j)} for j in range(stages)]
    )

    def cols(col):
        return pl.ds(pl.multiple_of(col * feat, feat), feat)

    base = []
    total = 0
    for stage in range(stages):
        base.append(total)
        total += m >> (stage + 1)

    order = far_near(n)[2]
    waits = []

    def send_stage(k, stage):
        dst = flipped(s, k, n)
        source = part_ref if stage == 0 else acc_buf
        peer = across(stage)
        step = 2 ** (stage + 1)
        for i in range(m // step):
            col = lax.rem(peer + i * step, m)
            at = base[stage] + i
            copy = remote(
                source.at[dst, :, cols(col)],
                in_buf.at[at, k],
                rs_send.at[at, k],
                rs_recv.at[at, k],
                {"tp": peer},
            )
            copy.start()
            waits.append(copy)

    def sum_stage(k, stage):
        dst = flipped(s, k, n)
        source = part_ref if stage == 0 else acc_buf
        step = 2 ** (stage + 1)
        for i in range(m // step):
            col = lax.rem(t + i * step, m)
            at = base[stage] + i
            remote(
                source.at[dst, :, cols(col)],
                in_buf.at[at, k],
                rs_send.at[at, k],
                rs_recv.at[at, k],
                {"tp": across(stage)},
            ).wait_recv()
            mine = source[dst, :, cols(col)].astype(jnp.float32)
            acc_buf[dst, :, cols(col)] = (mine + in_buf[at, k].astype(jnp.float32)).astype(
                jnp.bfloat16
            )

    def send_home(k):
        dst = flipped(s, k, n)
        if k == 0:
            back_buf[s] = acc_buf[s, :, cols(t)]
            return
        copy = remote(
            acc_buf.at[dst, :, cols(t)],
            back_buf.at[s],
            a2a_send.at[k],
            a2a_recv.at[k],
            {"sp": dst},
        )
        copy.start()
        waits.append(copy)

    for k in order:
        send_stage(k, 0)
    for at in range(n + stages - 1):
        for stage in range(stages):
            if 0 <= at - stage < n:
                k = order[at - stage]
                sum_stage(k, stage)
                if stage + 1 < stages:
                    send_stage(k, stage + 1)
                else:
                    send_home(k)
    value = cot_ref[...].astype(jnp.float32)
    for k in [0] + order[:-1]:
        src = flipped(s, k, n)
        if k > 0:
            remote(
                acc_buf.at[src, :, cols(t)],
                back_buf.at[src],
                a2a_send.at[k],
                a2a_recv.at[k],
                {"sp": src},
            ).wait_recv()
        value = value + jnp.dot(
            pick_ref[src], back_buf[src], preferred_element_type=jnp.float32
        )
    out_ref[:, cols(t)] = value.astype(jnp.bfloat16)

    def share(stage, i, col):
        at = 2**stage - 1 + i
        return remote(
            out_ref.at[:, cols(col)],
            out_ref.at[:, cols(col)],
            ag_send.at[at],
            ag_recv.at[at],
            {"tp": partner(t, stage, m)},
        )

    def push(stage, i, col):
        copy = share(stage, i, col)
        copy.start()
        waits.append(copy)

    for stage in range(stages):
        push(stage, 0, t)
    for stage in range(stages):
        for i, col in enumerate(held_columns(partner(t, stage, m), stage, m)):
            share(stage, i, col).wait_recv()
            for later in range(stage + 1, stages):
                push(later, 2**stage + i, col)
    for copy in waits:
        copy.wait_send()


def bring_back(part, pick, output_gradient):
    n, m = lax.axis_size("sp"), lax.axis_size("tp")
    _, cap, width = part.shape
    rows, feat = output_gradient.shape
    vmem = pl.BlockSpec(memory_space=pltpu.VMEM)
    return pl.pallas_call(
        functools.partial(return_kernel, n, m),
        out_shape=jax.ShapeDtypeStruct((rows, width), jnp.bfloat16),
        in_specs=[vmem] * 3,
        out_specs=vmem,
        scratch_shapes=[
            pltpu.VMEM((m - 1, n, cap, feat), jnp.bfloat16),
            pltpu.VMEM((n, cap, width), jnp.bfloat16),
            pltpu.VMEM((n, cap, feat), jnp.bfloat16),
            pltpu.SemaphoreType.DMA((m - 1, n)),
            pltpu.SemaphoreType.DMA((m - 1, n)),
            pltpu.SemaphoreType.DMA((n,)),
            pltpu.SemaphoreType.DMA((n,)),
            pltpu.SemaphoreType.DMA((m - 1,)),
            pltpu.SemaphoreType.DMA((m - 1,)),
        ],
        compiler_params=pltpu.CompilerParams(collective_id=2, has_side_effects=True),
        name="bring_back",
    )(part, pick, output_gradient)


def tail_kernel(
    n,
    decay_ref,
    input_ref,
    part_ref,
    grad_ref,
    sum_ref,
    gain_buf,
    car_send,
    car_buf,
    part_buf,
    pair_buf,
    part_ssem,
    part_rsem,
    car_ssem,
    car_rsem,
):
    s = lax.axis_index("sp")
    greet([{"sp": lax.rem(s + k, n)} for k in range(1, n)])
    beside = flipped(s, 1, n)
    half = n // 2
    order = [half - 1 - j for j in range(half)]
    near = {}
    for j in order:
        dst = flipped(s, 2 * j + 1, n)
        near[j] = remote(
            part_ref.at[dst], part_buf.at[j], part_ssem.at[j], part_rsem.at[j], {"sp": beside}
        )
        near[j].start()
    decay = decay_ref[...]
    gain, term = local_scan(shifted(decay, 1, 1.0, True), input_ref[...], True)
    gain_buf[...] = gain
    grad_ref[...] = term
    car_send[0:1] = decay[0:1] * gain[0:1]
    car_send[1:2] = decay[0:1] * term[0:1]
    carries = []
    for k in range(1, n):
        copy = remote(
            car_send, car_buf.at[k], car_ssem.at[k], car_rsem.at[k], {"sp": lax.rem(s + k, n)}
        )
        copy.start()
        carries.append(copy)
    far = {}
    for j in order:
        near[j].wait_recv()
        home = flipped(s, 2 * j, n)
        both = part_ref[home].astype(jnp.float32) + part_buf[j].astype(jnp.float32)
        if j == 0:
            sum_ref[...] = both
            continue
        pair_buf[j] = both.astype(jnp.bfloat16)
        at = half + j
        far[j] = remote(
            pair_buf.at[j], part_buf.at[at], part_ssem.at[at], part_rsem.at[at], {"sp": home}
        )
        far[j].start()
    for copy in carries:
        copy.wait()
    carry = jnp.zeros((1, gain_buf.shape[1]), jnp.float32)
    for k in range(1, n):
        carry = jnp.where(k > s, car_buf[k, 0:1] * carry + car_buf[k, 1:2], carry)
    grad_ref[...] = grad_ref[...] + gain_buf[...] * carry
    for j in order[:-1]:
        far[j].wait_recv()
        sum_ref[...] += part_buf[half + j].astype(jnp.float32)
    for j in order:
        near[j].wait_send()
    for j in order[:-1]:
        far[j].wait_send()


def tail(decay, state_in, part):
    n = lax.axis_size("sp")
    rows, channels = decay.shape
    vmem = pl.BlockSpec(memory_space=pltpu.VMEM)
    return pl.pallas_call(
        functools.partial(tail_kernel, n),
        out_shape=(
            jax.ShapeDtypeStruct((rows, channels), jnp.float32),
            jax.ShapeDtypeStruct(part.shape[1:], jnp.float32),
        ),
        in_specs=[vmem] * 3,
        out_specs=(vmem,) * 2,
        scratch_shapes=[
            pltpu.VMEM((rows, channels), jnp.float32),
            pltpu.VMEM((2, channels), jnp.float32),
            pltpu.VMEM((n, 2, channels), jnp.float32),
            pltpu.VMEM(part.shape, part.dtype),
            pltpu.VMEM((n // 2,) + part.shape[1:], part.dtype),
            pltpu.SemaphoreType.DMA((n,)),
            pltpu.SemaphoreType.DMA((n,)),
            pltpu.SemaphoreType.DMA((n,)),
            pltpu.SemaphoreType.DMA((n,)),
        ],
        compiler_params=pltpu.CompilerParams(collective_id=1, has_side_effects=True),
        name="tail",
    )(decay, state_in, part)


def gelu_parts(output_gate_logits):
    gate_float = output_gate_logits.astype(jnp.float32)
    return jax.jvp(jax.nn.gelu, (gate_float,), (jnp.ones_like(gate_float),))


def expert_backward(inputs, cotangent, gate_weight, up_weight, down_weight):
    gate_act = jnp.dot(inputs, gate_weight, preferred_element_type=jnp.float32)
    up_act = jnp.dot(inputs, up_weight, preferred_element_type=jnp.float32)
    sigmoid_gate = jax.nn.sigmoid(gate_act)
    silu_act = gate_act * sigmoid_gate
    hidden = (silu_act * up_act).astype(jnp.bfloat16)
    d_hidden = lax.dot_general(
        cotangent, down_weight, (((1,), (1,)), ((), ())), preferred_element_type=jnp.float32
    )
    grad_down = lax.dot_general(
        hidden, cotangent, (((0,), (0,)), ((), ())), preferred_element_type=jnp.float32
    )
    d_gate = (d_hidden * up_act * sigmoid_gate * (1.0 + gate_act * (1.0 - sigmoid_gate))).astype(
        jnp.bfloat16
    )
    d_up = (d_hidden * silu_act).astype(jnp.bfloat16)
    grad_gate = lax.dot_general(
        inputs, d_gate, (((0,), (0,)), ((), ())), preferred_element_type=jnp.float32
    )
    grad_up = lax.dot_general(
        inputs, d_up, (((0,), (0,)), ((), ())), preferred_element_type=jnp.float32
    )
    partial_value = lax.dot_general(
        d_gate, gate_weight, (((1,), (1,)), ((), ())), preferred_element_type=jnp.float32
    )
    partial_value = partial_value + lax.dot_general(
        d_up, up_weight, (((1,), (1,)), ((), ())), preferred_element_type=jnp.float32
    )
    return (
        grad_gate.astype(jnp.bfloat16),
        grad_up.astype(jnp.bfloat16),
        grad_down.astype(jnp.bfloat16),
        partial_value,
    )


def per_device(
    middle_stream,
    output_gradient,
    routes,
    chosen_expert_weight,
    expert_gate_weight,
    expert_up_weight,
    expert_down_weight,
    recurrent_output_weight,
    recurrence_input,
    output_gate_logits,
    recurrence_gate_weight,
    input_gate_weight,
    channel_decay_param,
    extra_log_decay,
):
    rows_dev = middle_stream.shape[0]
    top_count = routes.shape[1]
    experts = lax.axis_size("sp")
    capacity = 3 * top_count * rows_dev // (2 * experts)
    feat_width = middle_stream.shape[1]
    choice = routes.T
    expert_ids = jnp.arange(experts, dtype=jnp.int32)
    named = [(choice[k][None, :] == expert_ids[:, None]) for k in range(top_count)]
    named_any = sum(part.astype(jnp.bfloat16) for part in named)
    position = jnp.arange(rows_dev, dtype=jnp.int32)
    earlier = (position[:, None] < position[None, :]).astype(jnp.bfloat16)
    rank = jnp.dot(named_any, earlier, preferred_element_type=jnp.float32).astype(jnp.int32)
    slot_ids = jnp.arange(experts * capacity, dtype=jnp.int32)
    picks = []
    for k in range(top_count):
        slot = jnp.sum(
            jnp.where(named[k], rank + expert_ids[:, None] * capacity, 0), axis=0, keepdims=True
        )
        picks.append((slot_ids[:, None] == slot).astype(jnp.bfloat16))
    pick_any = sum(picks)
    pick_both = jnp.concatenate(picks, axis=1)
    pair_cot = (
        chosen_expert_weight.T[:, :, None] * output_gradient.astype(jnp.float32)[None]
    ).astype(jnp.bfloat16)
    pair_cot = pair_cot.reshape(-1, feat_width)
    send_rows = jnp.dot(pick_any, middle_stream, preferred_element_type=jnp.bfloat16)
    send_cot = jnp.dot(pick_both, pair_cot, preferred_element_type=jnp.bfloat16)
    channels = recurrence_input.shape[1]
    block_width = recurrence_gate_weight.shape[1]
    local_blocks = channels // block_width
    first_block = lax.axis_index("tp") * local_blocks
    recall_weight = lax.dynamic_slice_in_dim(recurrence_gate_weight, first_block, local_blocks, 0)
    admit_weight = lax.dynamic_slice_in_dim(input_gate_weight, first_block, local_blocks, 0)
    u_blocks = recurrence_input.reshape(rows_dev, local_blocks, block_width)
    forget_gate = jax.nn.sigmoid(
        jnp.einsum(
            "tnb,nbc->tnc", u_blocks, recall_weight, preferred_element_type=jnp.float32
        ).reshape(rows_dev, channels)
    )
    admit_gate = jax.nn.sigmoid(
        jnp.einsum(
            "tnb,nbc->tnc", u_blocks, admit_weight, preferred_element_type=jnp.float32
        ).reshape(rows_dev, channels)
    )
    baseline_rate = jax.nn.softplus(-channel_decay_param)
    decay_logarithm = -8.0 * forget_gate * baseline_rate[None, :] + extra_log_decay
    decay_step = jnp.exp(decay_logarithm)
    input_scale = jnp.sqrt(-jnp.expm1(2.0 * decay_logarithm))
    u_float = recurrence_input.astype(jnp.float32)
    driven = u_float * admit_gate * input_scale
    recv_rows, recv_cot, states, prev_states = dispatch(
        send_rows.reshape(experts, capacity, feat_width),
        send_cot.reshape(experts, capacity, feat_width),
        decay_step,
        driven,
    )
    row_width = recv_rows.shape[2]
    inputs = recv_rows.reshape(-1, row_width)
    cotangent = recv_cot.reshape(-1, row_width)
    grad_gate, grad_up, grad_down, partial_value = expert_backward(
        inputs, cotangent, expert_gate_weight[0], expert_up_weight[0], expert_down_weight[0]
    )
    grad_full = bring_back(
        partial_value.astype(jnp.bfloat16).reshape(experts, capacity, row_width),
        pick_any.reshape(experts, capacity, rows_dev).transpose(0, 2, 1),
        output_gradient,
    )
    mixer_grad = jnp.dot(grad_full, recurrent_output_weight, preferred_element_type=jnp.float32)
    gelu_val, gelu_der = gelu_parts(output_gate_logits)
    lru_out = (states * gelu_val).astype(jnp.bfloat16)
    gop_part = lax.dot_general(
        grad_full, lru_out, (((0,), (0,)), ((), ())), preferred_element_type=jnp.float32
    ).astype(jnp.bfloat16)
    gop_part = gop_part.reshape(experts, -1, channels)
    grad_gate_pre = mixer_grad * states * gelu_der
    state_in = mixer_grad * gelu_val
    state_grad, grad_out_proj = tail(decay_step, state_in, gop_part)
    d_log = state_grad * (
        prev_states * decay_step - u_float * admit_gate * decay_step * decay_step / input_scale
    )
    d_recall = (d_log * (-8.0 * baseline_rate[None, :]) * forget_gate * (1.0 - forget_gate)).astype(
        jnp.bfloat16
    )
    d_admit = (state_grad * u_float * input_scale * admit_gate * (1.0 - admit_gate)).astype(
        jnp.bfloat16
    )
    back_recall = jnp.einsum(
        "tnc,nbc->tnb",
        d_recall.reshape(rows_dev, local_blocks, block_width),
        recall_weight,
        preferred_element_type=jnp.float32,
    )
    back_admit = jnp.einsum(
        "tnc,nbc->tnb",
        d_admit.reshape(rows_dev, local_blocks, block_width),
        admit_weight,
        preferred_element_type=jnp.float32,
    )
    grad_input = state_grad * admit_gate * input_scale + (back_recall + back_admit).reshape(
        rows_dev, channels
    )
    return (
        grad_gate[None],
        grad_up[None],
        grad_down[None],
        grad_out_proj,
        grad_input,
        grad_gate_pre,
    )


def solution(mesh):
    placed = (
        P("sp", "tp"),
        P("sp", "tp"),
        P("sp", None),
        P("sp", None),
        P("sp", None, "tp"),
        P("sp", None, "tp"),
        P("sp", "tp", None),
        P(None, "tp"),
        P("sp", "tp"),
        P("sp", "tp"),
        P(),
        P(),
        P("tp"),
        P("sp", "tp"),
    )
    return jax.shard_map(
        per_device,
        mesh=mesh,
        in_specs=placed,
        out_specs=(
            P("sp", None, "tp"),
            P("sp", None, "tp"),
            P("sp", "tp", None),
            P("sp", "tp"),
            P("sp", "tp"),
            P("sp", "tp"),
        ),
        check_vma=False,
    )
```
